32 devices in a mesh: grp: 2 (over x), sp: 8 (over z, y), tp: 2 (over core).
Axes of the slice: x: 2, y: 2, z: 4, core: 2. Of those that a mesh axis runs over, the one named last changes fastest.
Arguments:
- probe_preactivation: bfloat16 [4096, 2048], P(('grp', 'sp'), 'tp'), parts along dimension 0, may hold values from -6 to 6
- retention_preactivation: bfloat16 [4096, 2048], P(('grp', 'sp'), 'tp'), parts along dimension 0, may hold values from -5 to 5.5
- source_entries: bfloat16 [4096, 2048], P(('grp', 'sp'), 'tp'), parts along dimension 0, may hold values from -6 to 6
- extra_log_retention: float32 [4096, 16], P(('grp', 'sp'), 'tp'), parts along dimension 0, may hold values from -1.39 to 0
- retention_slack: float32 [2048], P('tp'), as said below
- group_normalizer_gain: float32 [128], replicated, may hold values from 0.1 to 1.9
- readout_mapping_matrix: bfloat16 [2048, 2048], P('tp'), may hold values from -0.125 to 0.125
Outputs:
- mixed: bfloat16 [4096, 2048], P(('grp', 'sp', 'tp')), parts along dimension 0
The draws below stay inside these ranges and needn't reach their ends.
There are 2 independent parts, one for each index of `grp`. The reference program is written for one: setup_inputs(seed, part) draws one part's arguments, and reference() takes and returns one part's arrays. A program takes and returns all parts, laid end to end along the dimension named above; an argument that names none is the same for every part. Nothing has to cross between parts.
Inputs may be any that keep to these rules, and one draw needn't show every extreme that they name: `retention_slack`: every entry is positive.
All inputs are finite; a program needn't handle non-finite values.
Results may differ from the reference program's by a relative error of at most 0.014.
Values may be sent and summed in bfloat16 or wider, within the bound.
A program may use at most 128 MiB of HBM per device.

```python
import math
import jax
import jax.numpy as jnp
from jax import lax

D = 2048
RECURRENT_HEADS = 16
HEAD = 128
SPAN = 128
TOK_DEV = 256
CHANNELS = 2048
SEQ = 2048
TOTAL_TOKENS = 2048


def draw_retention_preactivation(key, part):
    primary_random_key, secondary_random_key = jax.random.split(jax.random.fold_in(key, 11))
    baseline = jnp.clip(jax.random.normal(primary_random_key, (TOTAL_TOKENS, CHANNELS), jnp.float32), -4.0, 4.0)
    block_len = TOK_DEV // 2
    shifts = jax.random.uniform(secondary_random_key, (TOTAL_TOKENS // block_len, 1), jnp.float32, -1.0, 1.5)
    shifts = jnp.repeat(shifts, block_len, axis=0)
    return (baseline + shifts).astype(jnp.bfloat16)


def draw_retention_slack(key, part):
    primary_random_key, secondary_random_key, third_key = jax.random.split(jax.random.fold_in(key, 23), 3)
    shuffled = jax.random.permutation(primary_random_key, RECURRENT_HEADS)
    fast_count = RECURRENT_HEADS // 2
    low_end = math.log(0.04)
    high_end = math.log(0.07)
    fast_head = jnp.repeat(shuffled < fast_count, HEAD)
    quick_room = jnp.exp(jax.random.uniform(secondary_random_key, (CHANNELS,), jnp.float32, low_end, high_end))
    slow_room = jnp.exp(jax.random.uniform(third_key, (CHANNELS,), jnp.float32, math.log(0.2), 0.0)) / SEQ
    return jnp.where(fast_head, quick_room, slow_room).astype(jnp.float32)


def draw_extra_log_retention(key, part):
    primary_random_key, secondary_random_key = jax.random.split(jax.random.fold_in(key, 37))
    segment_rows = jax.random.randint(primary_random_key, (2, RECURRENT_HEADS), 0, TOTAL_TOKENS)
    segment_length = jax.random.uniform(secondary_random_key, (2, RECURRENT_HEADS), jnp.float32, math.log(0.5), math.log(0.8))
    token_positions = jnp.arange(TOTAL_TOKENS, dtype=jnp.int32)[:, None]
    final_output = jnp.where(token_positions == segment_rows[0][None], segment_length[0][None], 0.0)
    final_output = final_output + jnp.where(token_positions == segment_rows[1][None], segment_length[1][None], 0.0)
    return final_output.astype(jnp.float32)


def steps_of(rng, extent, shards, low, high):
    factor_of = 1.0
    for dim, blocks in shards:
        heights = jax.random.uniform(jax.random.fold_in(jax.random.fold_in(rng, 6), dim), (blocks,), jnp.float32, low / len(shards), high / len(shards))
        factor_of = factor_of * jnp.repeat(jnp.exp(heights), extent[dim] // blocks).reshape((-1,) + (1,) * (len(extent) - 1 - dim))
    return factor_of


def noise(rng, dims, deviation, reach, shards=(), kind=jnp.bfloat16):
    values = deviation * jax.random.normal(rng, dims, jnp.float32)
    if shards:
        values = values * steps_of(rng, dims, shards, -0.22, 0.18)
    return jnp.clip(values, -reach, reach).astype(kind)


def setup_inputs(seed: int = 0, part: int = 0) -> dict:
    streams_of = jax.random.split(jax.random.key(seed), 8)
    own_keys = jax.random.split(jax.random.fold_in(streams_of[7], part), 8)
    probe_preactivation = noise(own_keys[0], (TOTAL_TOKENS, CHANNELS), 1.0, 6.0, ((0, 8), (1, 2)))
    retention_preactivation = draw_retention_preactivation(jax.random.fold_in(jax.random.fold_in(streams_of[7], part), 71), part)
    source_entries = noise(own_keys[2], (TOTAL_TOKENS, CHANNELS), 1.0, 6.0, ((0, 8), (1, 2)))
    extra_log_retention = draw_extra_log_retention(jax.random.fold_in(jax.random.fold_in(streams_of[7], part), 71), part)
    retention_slack = draw_retention_slack(jax.random.fold_in(streams_of[7], 71), part)
    group_normalizer_gain = jnp.clip(1.0 + 0.18 * jax.random.normal(streams_of[5], (HEAD,), jnp.float32), 0.1, 1.9)
    readout_mapping_matrix = noise(streams_of[6], (CHANNELS, D), CHANNELS ** -0.5, 0.125, ((0, 2),))
    return {"probe_preactivation": probe_preactivation, "retention_preactivation": retention_preactivation, "source_entries": source_entries, "extra_log_retention": extra_log_retention, "retention_slack": retention_slack, "group_normalizer_gain": group_normalizer_gain, "readout_mapping_matrix": readout_mapping_matrix}


TOP_PRECISION = lax.Precision.HIGHEST

def rounded_values(value):
    return lax.optimization_barrier(value.astype(jnp.bfloat16)).astype(jnp.float32)

def assemble_arguments(probe_preactivation, retention_preactivation, source_entries, extra_log_retention, retention_slack):
    tokens_here = probe_preactivation.shape[0]
    group_count = extra_log_retention.shape[1]
    head_dim = probe_preactivation.shape[1] // group_count
    probe_matrix = jax.nn.silu(probe_preactivation.astype(jnp.float32)).reshape(tokens_here, group_count, head_dim)
    scaled_address_matrix = (retention_slack * jax.nn.sigmoid(-retention_preactivation.astype(jnp.float32))).reshape(tokens_here, group_count, head_dim)
    log_retention_factor = jnp.log1p(-scaled_address_matrix) + extra_log_retention[:, :, None]
    content_matrix = source_entries.astype(jnp.float32).reshape(tokens_here, group_count, head_dim)
    return (probe_matrix, scaled_address_matrix, content_matrix, log_retention_factor)

def block_pass(carried_state, pieces):
    probe_matrix, scaled_address_matrix, content_matrix, log_retention_factor = pieces
    span_len = probe_matrix.shape[0]
    running = jnp.cumsum(log_retention_factor, axis=0)
    raised_values = rounded_values(probe_matrix * jnp.exp(running))
    lowered = rounded_values(scaled_address_matrix * jnp.exp(-running))
    scores = jnp.einsum('thk,shk->hts', raised_values, lowered, precision=TOP_PRECISION)
    row_index = lax.broadcasted_iota(jnp.int32, (span_len, span_len), 0)
    col_index = lax.broadcasted_iota(jnp.int32, (span_len, span_len), 1)
    scores = rounded_values(jnp.where((row_index >= col_index)[None], scores, jnp.zeros_like(scores)))
    final_output = jnp.einsum('hts,shv->thv', scores, content_matrix, precision=TOP_PRECISION)
    final_output = final_output + jnp.einsum('csq,sqd->csd', raised_values, rounded_values(carried_state), precision=TOP_PRECISION)
    final_running_sum = running[-1]
    passed_state = rounded_values(scaled_address_matrix * jnp.exp(final_running_sum[None] - running))
    carried_state = jnp.exp(final_running_sum)[:, :, None] * carried_state + jnp.einsum('wcf,wcz->cfz', passed_state, content_matrix, precision=TOP_PRECISION)
    return (carried_state, final_output)

def finish(mixer_out, group_normalizer_gain):
    scale = lax.rsqrt(lax.optimization_barrier(jnp.mean(mixer_out * mixer_out, axis=-1, keepdims=True)) + 1e-06)
    normed = (mixer_out * scale * group_normalizer_gain).astype(jnp.bfloat16)
    return normed.reshape(mixer_out.shape[0], mixer_out.shape[1] * mixer_out.shape[2])

def reference(probe_preactivation, retention_preactivation, source_entries, extra_log_retention, retention_slack, group_normalizer_gain, readout_mapping_matrix):
    probe_matrix, scaled_address_matrix, content_matrix, log_retention_factor = assemble_arguments(probe_preactivation, retention_preactivation, source_entries, extra_log_retention, retention_slack)
    length = probe_matrix.shape[0]
    blocks = length // SPAN
    pieces = tuple((a.reshape(blocks, SPAN, RECURRENT_HEADS, HEAD) for a in (probe_matrix, scaled_address_matrix, content_matrix, log_retention_factor)))
    initial = jnp.zeros((RECURRENT_HEADS, HEAD, HEAD), jnp.float32)
    _, mixer_out = lax.scan(block_pass, initial, pieces)
    normed = finish(mixer_out.reshape(length, RECURRENT_HEADS, HEAD), group_normalizer_gain)
    return jnp.dot(normed, readout_mapping_matrix, preferred_element_type=jnp.float32).astype(jnp.bfloat16)
```

```python
import functools

import jax
import jax.numpy as jnp
from jax import lax
from jax.experimental import pallas as pl
from jax.experimental.pallas import tpu as pltpu
from jax.sharding import PartitionSpec as P

SPAN = 128
GROUP = 2
TILES = 4
MESH = pl.DeviceIdType.MESH
F32 = jnp.float32
BF16 = jnp.bfloat16


def dot(a, b, contract):
    return lax.dot_general(a, b, (contract, ((), ())), preferred_element_type=F32)


def kernel(
    n_sp,
    p_hbm,
    r_hbm,
    v_hbm,
    x_ref,
    slack_ref,
    gain_ref,
    w_hbm,
    out_ref,
    p_ref,
    r_ref,
    v_ref,
    w_ref,
    lifted,
    lowered,
    lfull,
    inner,
    local,
    decay,
    intra,
    swap_out,
    swap_in,
    chain_out,
    chain_in,
    enter,
    normed,
    acc,
    half_out,
    half_in,
    in_sem,
    w_sem,
    swap_send,
    swap_recv,
    chain_send,
    chain_recv,
    half_send,
    half_recv,
):
    tokens, channels = p_ref.shape
    heads = x_ref.shape[0]
    dim = channels // heads
    blocks = tokens // SPAN
    groups = heads // GROUP
    wide = w_ref.shape[1]
    tile = wide // TILES
    half = out_ref.shape[0]
    sp, tp = lax.axis_index("sp"), lax.axis_index("tp")
    pairs = n_sp // 2
    pair, odd = sp // 2, sp % 2
    mate = sp + 1 - 2 * odd
    first, last = pair == 0, pair == pairs - 1

    loads = []
    for g in range(groups):
        cols = pl.ds(g * GROUP * dim, GROUP * dim)
        loads.append(
            [
                pltpu.make_async_copy(src.at[:, cols], dst.at[:, cols], in_sem.at[g, i])
                for i, (src, dst) in enumerate(((r_hbm, r_ref), (v_hbm, v_ref), (p_hbm, p_ref)))
            ]
        )
        for c in loads[g]:
            c.start()
    w_loads = []
    for g in range(groups):
        rows = pl.ds(g * GROUP * dim, GROUP * dim)
        w_loads.append(pltpu.make_async_copy(w_hbm.at[rows, :], w_ref.at[rows, :], w_sem.at[g]))
        w_loads[g].start()

    barrier = pltpu.get_barrier_semaphore()
    pl.semaphore_signal(barrier, inc=1, device_id={"sp": mate}, device_id_type=MESH)
    pl.semaphore_signal(barrier, inc=1, device_id={"tp": 1 - tp}, device_id_type=MESH)

    @pl.when(jnp.logical_not(first))
    def _():
        pl.semaphore_signal(barrier, inc=1, device_id={"sp": sp - 2}, device_id_type=MESH)

    @pl.when(jnp.logical_not(last))
    def _():
        pl.semaphore_signal(barrier, inc=1, device_id={"sp": sp + 2}, device_id_type=MESH)

    @pl.when(first)
    def _():
        chain_in[...] = jnp.zeros_like(chain_in)

    extra = x_ref[...].T
    row = lax.broadcasted_iota(jnp.int32, (SPAN, SPAN), 0)
    col = lax.broadcasted_iota(jnp.int32, (SPAN, SPAN), 1)
    causal = row >= col
    tri = jnp.where(causal, 1.0, 0.0).astype(BF16)
    tri2 = jnp.concatenate([tri, tri], axis=1)
    tag = lax.broadcasted_iota(jnp.int32, (16, dim), 0) == 0

    def swap(h):
        return pltpu.make_async_remote_copy(
            swap_out.at[h],
            swap_in.at[h],
            swap_send.at[h],
            swap_recv.at[h],
            device_id={"sp": mate},
            device_id_type=MESH,
        )

    def chain(h):
        return pltpu.make_async_remote_copy(
            chain_out.at[h],
            chain_in.at[h],
            chain_send.at[h],
            chain_recv.at[h],
            device_id={"sp": jnp.minimum(sp + 2, n_sp - 2 + odd)},
            device_id_type=MESH,
        )

    def summarise(h):
        hs = slice(h * dim, (h + 1) * dim)
        slack = slack_ref[:, hs]
        state, offset = None, None
        for b in range(blocks):
            ts = slice(b * SPAN, (b + 1) * SPAN)
            keyed = slack * (0.5 - 0.5 * jnp.tanh(0.5 * r_ref[ts, hs].astype(F32)))
            log_decay = jnp.log(1.0 - keyed) + extra[ts, h : h + 1]
            high = log_decay.astype(BF16)
            low = (log_decay - high.astype(F32)).astype(BF16)
            running = dot(tri2, jnp.concatenate([high, low], axis=0), ((1,), (0,)))
            end = running[SPAN - 1 :, :]
            probe = p_ref[ts, hs].astype(F32)
            query = probe * (0.5 + 0.5 * jnp.tanh(0.5 * probe))
            raised = query * jnp.exp(running)
            lifted[ts, hs] = raised.astype(BF16)
            lowered[ts, hs] = (keyed * jnp.exp(-running)).astype(BF16)
            sent = (keyed * jnp.exp(end - running)).astype(BF16)
            fresh = dot(v_ref[ts, hs], sent, ((0,), (0,)))
            if b == 0:
                lfull[ts, hs] = raised.astype(BF16)
                state, offset = fresh, end
            else:
                lfull[ts, hs] = (raised * jnp.exp(offset)).astype(BF16)
                inner[h, b - 1] = state.astype(BF16)
                state, offset = jnp.exp(end) * state + fresh, offset + end
        local[h] = state
        total = jnp.exp(offset)
        decay[h] = jnp.broadcast_to(total, (8, dim))
        high = total.astype(BF16)
        low = (total - high.astype(F32)).astype(BF16)
        swap_out[h, :dim, :] = state.astype(BF16)
        swap_out[h, dim:, :] = jnp.where(tag, high.astype(F32), low.astype(F32)).astype(BF16)

    def pass_on(h):
        swap(h).wait_recv()
        other = swap_in[h, :dim, :].astype(F32)
        tail = swap_in[h, dim:, :].astype(F32)
        d_other = tail[0:1] + tail[1:2]
        own, d_own = local[h], decay[h, 0:1, :]
        is_odd = odd == 1
        s0 = jnp.where(is_odd, other, own)
        s1 = jnp.where(is_odd, own, other)
        d0 = jnp.where(is_odd, d_other, d_own)
        d1 = jnp.where(is_odd, d_own, d_other)
        before = chain_in[h].astype(F32)
        middle = d0 * before + s0
        chain_out[h] = (d1 * middle + s1).astype(BF16)

        @pl.when(jnp.logical_not(last))
        def _():
            chain(h).start()

        enter[h] = jnp.where(is_odd, middle, before).astype(BF16)

    def within(h):
        hs = slice(h * dim, (h + 1) * dim)
        for b in range(blocks):
            ts = slice(b * SPAN, (b + 1) * SPAN)
            up = lifted[ts, hs]
            scores = dot(up, lowered[ts, hs], ((1,), (1,)))
            scores = jnp.where(causal, scores, 0.0).astype(BF16)
            o = dot(scores, v_ref[ts, hs], ((1,), (0,)))
            if b > 0:
                o = o + dot(up, inner[h, b - 1], ((1,), (1,)))
            intra[ts, hs] = o

    gain = gain_ref[...]

    def close(h):
        hs = slice(h * dim, (h + 1) * dim)
        o = intra[:, hs] + dot(lfull[:, hs], enter[h], ((1,), (1,)))
        scale = lax.rsqrt(jnp.mean(o * o, axis=-1, keepdims=True) + 1e-6)
        normed[:, hs] = (o * scale * gain).astype(BF16)

    for g in range(groups):
        for c in loads[g]:
            c.wait()
        for h in range(g * GROUP, (g + 1) * GROUP):
            summarise(h)
        if g == 0:
            pl.semaphore_wait(barrier, 4 - first.astype(jnp.int32) - last.astype(jnp.int32))

        for h in range(g * GROUP, (g + 1) * GROUP):
            swap(h).start()

    @pl.when(first)
    def _():
        for h in range(heads):
            pass_on(h)

    for h in range(heads):
        within(h)

    theirs = pl.ds(pl.multiple_of((1 - tp) * half, half), half)
    mine = pl.ds(pl.multiple_of(tp * half, half), half)

    def exchange(t):
        ns = pl.ds(t * tile, tile)
        return pltpu.make_async_remote_copy(
            half_out.at[:, ns],
            half_in.at[:, ns],
            half_send.at[t],
            half_recv.at[t],
            device_id={"tp": 1 - tp},
            device_id_type=MESH,
        )

    for g in range(groups):
        hs = range(g * GROUP, (g + 1) * GROUP)

        @pl.when(jnp.logical_not(first))
        def _():
            for h in hs:
                chain(h).wait_recv()
                pass_on(h)

        for h in hs:
            close(h)
        w_loads[g].wait()
        ks = slice(g * GROUP * dim, (g + 1) * GROUP * dim)
        if g < groups - 1:
            for t in range(TILES):
                ns = slice(t * tile, (t + 1) * tile)
                part = dot(normed[:, ks], w_ref[ks, ns], ((1,), (0,)))
                acc[:, ns] = part if g == 0 else acc[:, ns] + part
        else:
            for t in range(TILES):
                ns = slice(t * tile, (t + 1) * tile)
                part = dot(normed[theirs, ks], w_ref[ks, ns], ((1,), (0,)))
                if groups > 1:
                    part = part + acc[theirs, ns]
                half_out[:, ns] = part.astype(BF16)
                exchange(t).start()
            for t in range(TILES):
                ns = slice(t * tile, (t + 1) * tile)
                part = dot(normed[mine, ks], w_ref[ks, ns], ((1,), (0,)))
                if groups > 1:
                    part = part + acc[mine, ns]
                exchange(t).wait_recv()
                out_ref[:, ns] = (part + half_in[:, ns].astype(F32)).astype(BF16)

    for h in range(heads):
        swap(h).wait_send()

    @pl.when(jnp.logical_not(last))
    def _():
        for h in range(heads):
            chain(h).wait_send()

    for t in range(TILES):
        exchange(t).wait_send()


def body(n_sp, n_tp, p, r, v, x, slack, gain, w):
    tokens, channels = p.shape
    heads = x.shape[1]
    dim = channels // heads
    blocks = tokens // SPAN
    groups = heads // GROUP
    wide = w.shape[1]
    half = tokens // n_tp
    vmem = pl.BlockSpec(memory_space=pltpu.VMEM)
    hbm = pl.BlockSpec(memory_space=pl.ANY)
    dma = pltpu.SemaphoreType.DMA
    return pl.pallas_call(
        functools.partial(kernel, n_sp),
        out_shape=jax.ShapeDtypeStruct((half, wide), BF16),
        in_specs=[hbm, hbm, hbm, vmem, vmem, vmem, hbm],
        out_specs=vmem,
        scratch_shapes=[
            pltpu.VMEM((tokens, channels), BF16),
            pltpu.VMEM((tokens, channels), BF16),
            pltpu.VMEM((tokens, channels), BF16),
            pltpu.VMEM(w.shape, BF16),
            pltpu.VMEM((tokens, channels), BF16),
            pltpu.VMEM((tokens, channels), BF16),
            pltpu.VMEM((tokens, channels), BF16),
            pltpu.VMEM((heads, max(blocks - 1, 1), dim, dim), BF16),
            pltpu.VMEM((heads, dim, dim), F32),
            pltpu.VMEM((heads, 8, dim), F32),
            pltpu.VMEM((tokens, channels), F32),
            pltpu.VMEM((heads, dim + 16, dim), BF16),
            pltpu.VMEM((heads, dim + 16, dim), BF16),
            pltpu.VMEM((heads, dim, dim), BF16),
            pltpu.VMEM((heads, dim, dim), BF16),
            pltpu.VMEM((heads, dim, dim), BF16),
            pltpu.VMEM((tokens, channels), BF16),
            pltpu.VMEM((tokens, wide), F32),
            pltpu.VMEM((half, wide), BF16),
            pltpu.VMEM((half, wide), BF16),
            dma((groups, 3)),
            dma((groups,)),
            dma((heads,)),
            dma((heads,)),
            dma((heads,)),
            dma((heads,)),
            dma((TILES,)),
            dma((TILES,)),
        ],
        compiler_params=pltpu.CompilerParams(
            collective_id=0, has_side_effects=True, vmem_limit_bytes=60 * 2**20
        ),
    )(p, r, v, x.T, slack.reshape(1, channels), gain.reshape(1, dim), w)


def solution(mesh):
    return jax.shard_map(
        functools.partial(body, mesh.shape["sp"], mesh.shape["tp"]),
        mesh=mesh,
        in_specs=(
            P(("grp", "sp"), "tp"),
            P(("grp", "sp"), "tp"),
            P(("grp", "sp"), "tp"),
            P(("grp", "sp"), "tp"),
            P("tp"),
            P(),
            P("tp", None),
        ),
        out_specs=P(("grp", "sp", "tp"), None),
        check_vma=False,
    )
```

```python
import functools

import jax
import jax.numpy as jnp
from jax import lax
from jax.experimental import pallas as pl
from jax.experimental.pallas import tpu as pltpu
from jax.sharding import PartitionSpec as P

SPAN = 128
GROUP = 2
TILES = 4
PIECES = 2
MESH = pl.DeviceIdType.MESH
F32 = jnp.float32
BF16 = jnp.bfloat16


def dot(a, b, contract):
    return lax.dot_general(a, b, (contract, ((), ())), preferred_element_type=F32)


def kernel(
    n_sp,
    p_hbm,
    r_hbm,
    v_hbm,
    x_ref,
    slack_ref,
    gain_ref,
    w_hbm,
    out_ref,
    p_ref,
    r_ref,
    v_ref,
    w_ref,
    lifted,
    lowered,
    lfull,
    inner,
    local,
    decay,
    intra,
    swap_out,
    swap_in,
    chain_out,
    chain_in,
    enter,
    normed,
    acc,
    half_out,
    half_in,
    in_sem,
    w_sem,
    swap_send,
    swap_recv,
    chain_send,
    chain_recv,
    half_send,
    half_recv,
):
    tokens, channels = p_ref.shape
    heads = x_ref.shape[0]
    dim = channels // heads
    blocks = tokens // SPAN
    groups = heads // GROUP
    wide = w_ref.shape[1]
    tile = wide // TILES
    half = out_ref.shape[0]
    sp, tp = lax.axis_index("sp"), lax.axis_index("tp")
    pairs = n_sp // 2
    pair, odd = sp // 2, sp % 2
    mate = sp + 1 - 2 * odd
    first, last = pair == 0, pair == pairs - 1

    loads = []
    for g in range(groups):
        cols = pl.ds(g * GROUP * dim, GROUP * dim)
        loads.append(
            [
                pltpu.make_async_copy(src.at[:, cols], dst.at[:, cols], in_sem.at[g, i])
                for i, (src, dst) in enumerate(((r_hbm, r_ref), (v_hbm, v_ref), (p_hbm, p_ref)))
            ]
        )
        for c in loads[g]:
            c.start()
    w_loads = []
    for g in range(groups):
        rows = pl.ds(g * GROUP * dim, GROUP * dim)
        w_loads.append(pltpu.make_async_copy(w_hbm.at[rows, :], w_ref.at[rows, :], w_sem.at[g]))
        w_loads[g].start()

    barrier = pltpu.get_barrier_semaphore()
    pl.semaphore_signal(barrier, inc=1, device_id={"sp": mate}, device_id_type=MESH)
    pl.semaphore_signal(barrier, inc=1, device_id={"tp": 1 - tp}, device_id_type=MESH)

    @pl.when(jnp.logical_not(first))
    def _():
        pl.semaphore_signal(barrier, inc=1, device_id={"sp": sp - 2}, device_id_type=MESH)

    @pl.when(jnp.logical_not(last))
    def _():
        pl.semaphore_signal(barrier, inc=1, device_id={"sp": sp + 2}, device_id_type=MESH)

    @pl.when(first)
    def _():
        chain_in[...] = jnp.zeros_like(chain_in)

    extra = x_ref[...].T
    row = lax.broadcasted_iota(jnp.int32, (SPAN, SPAN), 0)
    col = lax.broadcasted_iota(jnp.int32, (SPAN, SPAN), 1)
    causal = row >= col
    tri = jnp.where(causal, 1.0, 0.0).astype(BF16)
    tri2 = jnp.concatenate([tri, tri], axis=1)
    tag = lax.broadcasted_iota(jnp.int32, (16, dim), 0) == 0

    def swap(h):
        return pltpu.make_async_remote_copy(
            swap_out.at[h],
            swap_in.at[h],
            swap_send.at[h],
            swap_recv.at[h],
            device_id={"sp": mate},
            device_id_type=MESH,
        )

    def chain(h, c):
        rows = pl.ds(c * (dim // PIECES), dim // PIECES)
        return pltpu.make_async_remote_copy(
            chain_out.at[h, rows],
            chain_in.at[h, rows],
            chain_send.at[h, c],
            chain_recv.at[h, c],
            device_id={"sp": jnp.minimum(sp + 2, n_sp - 2 + odd)},
            device_id_type=MESH,
        )

    def summarise(h):
        hs = slice(h * dim, (h + 1) * dim)
        slack = slack_ref[:, hs]
        state, offset = None, None
        for b in range(blocks):
            ts = slice(b * SPAN, (b + 1) * SPAN)
            keyed = slack * (0.5 - 0.5 * jnp.tanh(0.5 * r_ref[ts, hs].astype(F32)))
            log_decay = jnp.log(1.0 - keyed) + extra[ts, h : h + 1]
            high = log_decay.astype(BF16)
            low = (log_decay - high.astype(F32)).astype(BF16)
            running = dot(tri2, jnp.concatenate([high, low], axis=0), ((1,), (0,)))
            end = running[SPAN - 1 :, :]
            probe = p_ref[ts, hs].astype(F32)
            query = probe * (0.5 + 0.5 * jnp.tanh(0.5 * probe))
            raised = query * jnp.exp(running)
            lifted[ts, hs] = raised.astype(BF16)
            lowered[ts, hs] = (keyed * jnp.exp(-running)).astype(BF16)
            sent = (keyed * jnp.exp(end - running)).astype(BF16)
            fresh = dot(v_ref[ts, hs], sent, ((0,), (0,)))
            if b == 0:
                lfull[ts, hs] = raised.astype(BF16)
                state, offset = fresh, end
            else:
                lfull[ts, hs] = (raised * jnp.exp(offset)).astype(BF16)
                inner[h, b - 1] = state.astype(BF16)
                state, offset = jnp.exp(end) * state + fresh, offset + end
        local[h] = state
        total = jnp.exp(offset)
        decay[h] = jnp.broadcast_to(total, (8, dim))
        high = total.astype(BF16)
        low = (total - high.astype(F32)).astype(BF16)
        swap_out[h, :dim, :] = state.astype(BF16)
        swap_out[h, dim:, :] = jnp.where(tag, high.astype(F32), low.astype(F32)).astype(BF16)

    def pass_on(h, arrival):
        swap(h).wait_recv()
        tail = swap_in[h, dim:, :].astype(F32)
        d_other, d_own = tail[0:1] + tail[1:2], decay[h, 0:1, :]
        is_odd = odd == 1
        d0 = jnp.where(is_odd, d_other, d_own)
        d1 = jnp.where(is_odd, d_own, d_other)
        for c in range(PIECES):
            rows = pl.ds(c * (dim // PIECES), dim // PIECES)
            other, own = swap_in[h, rows, :].astype(F32), local[h, rows, :]
            s0 = jnp.where(is_odd, other, own)
            s1 = jnp.where(is_odd, own, other)
            if arrival:
                chain(h, c).wait_recv()
            before = chain_in[h, rows, :].astype(F32)
            middle = d0 * before + s0
            chain_out[h, rows, :] = (d1 * middle + s1).astype(BF16)

            @pl.when(jnp.logical_not(last))
            def _():
                chain(h, c).start()

            enter[h, rows, :] = jnp.where(is_odd, middle, before).astype(BF16)

    def within(h):
        hs = slice(h * dim, (h + 1) * dim)
        for b in range(blocks):
            ts = slice(b * SPAN, (b + 1) * SPAN)
            up = lifted[ts, hs]
            scores = dot(up, lowered[ts, hs], ((1,), (1,)))
            scores = jnp.where(causal, scores, 0.0).astype(BF16)
            o = dot(scores, v_ref[ts, hs], ((1,), (0,)))
            if b > 0:
                o = o + dot(up, inner[h, b - 1], ((1,), (1,)))
            intra[ts, hs] = o

    gain = gain_ref[...]

    def close(h):
        hs = slice(h * dim, (h + 1) * dim)
        o = intra[:, hs] + dot(lfull[:, hs], enter[h], ((1,), (1,)))
        scale = lax.rsqrt(jnp.mean(o * o, axis=-1, keepdims=True) + 1e-6)
        normed[:, hs] = (o * scale * gain).astype(BF16)

    for g in range(groups):
        for c in loads[g]:
            c.wait()
        for h in range(g * GROUP, (g + 1) * GROUP):
            summarise(h)
        if g == 0:
            pl.semaphore_wait(barrier, 4 - first.astype(jnp.int32) - last.astype(jnp.int32))

        for h in range(g * GROUP, (g + 1) * GROUP):
            swap(h).start()

    for h in range(heads):
        within(h)

        @pl.when(first)
        def _():
            pass_on(h, False)

    theirs = pl.ds(pl.multiple_of((1 - tp) * half, half), half)
    mine = pl.ds(pl.multiple_of(tp * half, half), half)

    def exchange(t):
        ns = pl.ds(t * tile, tile)
        return pltpu.make_async_remote_copy(
            half_out.at[:, ns],
            half_in.at[:, ns],
            half_send.at[t],
            half_recv.at[t],
            device_id={"tp": 1 - tp},
            device_id_type=MESH,
        )

    for g in range(groups):
        hs = range(g * GROUP, (g + 1) * GROUP)

        ahead = range(0 if g == 0 else (g + 1) * GROUP, min(g + 2, groups) * GROUP)

        @pl.when(jnp.logical_and(jnp.logical_not(first), jnp.logical_not(last)))
        def _():
            for h in ahead:
                pass_on(h, True)

        @pl.when(jnp.logical_and(jnp.logical_not(first), last))
        def _():
            for h in hs:
                pass_on(h, True)

        for h in hs:
            close(h)
        w_loads[g].wait()
        ks = slice(g * GROUP * dim, (g + 1) * GROUP * dim)
        if g < groups - 1:
            for t in range(TILES):
                ns = slice(t * tile, (t + 1) * tile)
                part = dot(normed[:, ks], w_ref[ks, ns], ((1,), (0,)))
                acc[:, ns] = part if g == 0 else acc[:, ns] + part
        else:
            for t in range(TILES):
                ns = slice(t * tile, (t + 1) * tile)
                part = dot(normed[theirs, ks], w_ref[ks, ns], ((1,), (0,)))
                if groups > 1:
                    part = part + acc[theirs, ns]
                half_out[:, ns] = part.astype(BF16)
                exchange(t).start()
            for t in range(TILES):
                ns = slice(t * tile, (t + 1) * tile)
                part = dot(normed[mine, ks], w_ref[ks, ns], ((1,), (0,)))
                if groups > 1:
                    part = part + acc[mine, ns]
                exchange(t).wait_recv()
                out_ref[:, ns] = (part + half_in[:, ns].astype(F32)).astype(BF16)

    for h in range(heads):
        swap(h).wait_send()

    @pl.when(jnp.logical_not(last))
    def _():
        for h in range(heads):
            for c in range(PIECES):
                chain(h, c).wait_send()

    for t in range(TILES):
        exchange(t).wait_send()


def body(n_sp, n_tp, p, r, v, x, slack, gain, w):
    tokens, channels = p.shape
    heads = x.shape[1]
    dim = channels // heads
    blocks = tokens // SPAN
    groups = heads // GROUP
    wide = w.shape[1]
    half = tokens // n_tp
    x, slack, gain = x.T, slack.reshape(1, channels), gain.reshape(1, dim)
    p, r, v, x, slack, gain, w = (
        pltpu.with_memory_space_constraint(a, pltpu.HBM) for a in (p, r, v, x, slack, gain, w)
    )
    vmem = pl.BlockSpec(memory_space=pltpu.VMEM)
    hbm = pl.BlockSpec(memory_space=pltpu.HBM)
    dma = pltpu.SemaphoreType.DMA
    return pl.pallas_call(
        functools.partial(kernel, n_sp),
        out_shape=jax.ShapeDtypeStruct((half, wide), BF16),
        in_specs=[hbm, hbm, hbm, vmem, vmem, vmem, hbm],
        out_specs=vmem,
        scratch_shapes=[
            pltpu.VMEM((tokens, channels), BF16),
            pltpu.VMEM((tokens, channels), BF16),
            pltpu.VMEM((tokens, channels), BF16),
            pltpu.VMEM(w.shape, BF16),
            pltpu.VMEM((tokens, channels), BF16),
            pltpu.VMEM((tokens, channels), BF16),
            pltpu.VMEM((tokens, channels), BF16),
            pltpu.VMEM((heads, max(blocks - 1, 1), dim, dim), BF16),
            pltpu.VMEM((heads, dim, dim), F32),
            pltpu.VMEM((heads, 8, dim), F32),
            pltpu.VMEM((tokens, channels), F32),
            pltpu.VMEM((heads, dim + 16, dim), BF16),
            pltpu.VMEM((heads, dim + 16, dim), BF16),
            pltpu.VMEM((heads, dim, dim), BF16),
            pltpu.VMEM((heads, dim, dim), BF16),
            pltpu.VMEM((heads, dim, dim), BF16),
            pltpu.VMEM((tokens, channels), BF16),
            pltpu.VMEM((tokens, wide), F32),
            pltpu.VMEM((half, wide), BF16),
            pltpu.VMEM((half, wide), BF16),
            dma((groups, 3)),
            dma((groups,)),
            dma((heads,)),
            dma((heads,)),
            dma((heads, PIECES)),
            dma((heads, PIECES)),
            dma((TILES,)),
            dma((TILES,)),
        ],
        compiler_params=pltpu.CompilerParams(
            collective_id=0, has_side_effects=True, vmem_limit_bytes=24 * 2**20
        ),
    )(p, r, v, x, slack, gain, w)


def solution(mesh):
    return jax.shard_map(
        functools.partial(body, mesh.shape["sp"], mesh.shape["tp"]),
        mesh=mesh,
        in_specs=(
            P(("grp", "sp"), "tp"),
            P(("grp", "sp"), "tp"),
            P(("grp", "sp"), "tp"),
            P(("grp", "sp"), "tp"),
            P("tp"),
            P(),
            P("tp", None),
        ),
        out_specs=P(("grp", "sp", "tp"), None),
        check_vma=False,
    )
```

```python
import functools

import jax
import jax.numpy as jnp
from jax import lax
from jax.experimental import pallas as pl
from jax.experimental.pallas import tpu as pltpu
from jax.sharding import PartitionSpec as P

SPAN = 128
GROUP = 2
TILES = 2
PIECES = 2
MESH = pl.DeviceIdType.MESH
F32 = jnp.float32
BF16 = jnp.bfloat16


def dot(a, b, contract):
    return lax.dot_general(a, b, (contract, ((), ())), preferred_element_type=F32)


def kernel(
    n_sp,
    p_hbm,
    r_hbm,
    v_hbm,
    x_ref,
    slack_ref,
    gain_ref,
    w_hbm,
    out_ref,
    p_ref,
    r_ref,
    v_ref,
    w_ref,
    lifted,
    lowered,
    lfull,
    inner,
    local,
    decay,
    intra,
    swap_out,
    swap_in,
    chain_out,
    chain_in,
    enter,
    normed,
    acc,
    half_out,
    half_in,
    in_sem,
    w_sem,
    swap_send,
    swap_recv,
    chain_send,
    chain_recv,
    half_send,
    half_recv,
):
    tokens, channels = p_ref.shape
    heads = x_ref.shape[0]
    dim = channels // heads
    blocks = tokens // SPAN
    groups = heads // GROUP
    wide = w_ref.shape[1]
    tile = wide // TILES
    half = out_ref.shape[0]
    sp, tp = lax.axis_index("sp"), lax.axis_index("tp")
    pairs = n_sp // 2
    pair, odd = sp // 2, sp % 2
    mate = sp + 1 - 2 * odd
    first, last = pair == 0, pair == pairs - 1

    loads = []
    for g in range(groups):
        cols = pl.ds(g * GROUP * dim, GROUP * dim)
        loads.append(
            [
                pltpu.make_async_copy(src.at[:, cols], dst.at[:, cols], in_sem.at[g, i])
                for i, (src, dst) in enumerate(((r_hbm, r_ref), (v_hbm, v_ref), (p_hbm, p_ref)))
            ]
        )
        for c in loads[g]:
            c.start()
    w_loads = []
    for g in range(groups):
        rows = pl.ds(g * GROUP * dim, GROUP * dim)
        w_loads.append(pltpu.make_async_copy(w_hbm.at[rows, :], w_ref.at[rows, :], w_sem.at[g]))
        w_loads[g].start()

    barrier = pltpu.get_barrier_semaphore()
    pl.semaphore_signal(barrier, inc=1, device_id={"sp": mate}, device_id_type=MESH)
    pl.semaphore_signal(barrier, inc=1, device_id={"tp": 1 - tp}, device_id_type=MESH)

    @pl.when(jnp.logical_not(first))
    def _():
        pl.semaphore_signal(barrier, inc=1, device_id={"sp": sp - 2}, device_id_type=MESH)

    @pl.when(jnp.logical_not(last))
    def _():
        pl.semaphore_signal(barrier, inc=1, device_id={"sp": sp + 2}, device_id_type=MESH)

    @pl.when(first)
    def _():
        chain_in[...] = jnp.zeros_like(chain_in)

    extra = x_ref[...].T
    row = lax.broadcasted_iota(jnp.int32, (SPAN, SPAN), 0)
    col = lax.broadcasted_iota(jnp.int32, (SPAN, SPAN), 1)
    causal = row >= col
    tri = jnp.where(causal, 1.0, 0.0).astype(BF16)
    tri2 = jnp.concatenate([tri, tri], axis=1)
    tag = lax.broadcasted_iota(jnp.int32, (16, dim), 0) == 0

    def swap(h):
        return pltpu.make_async_remote_copy(
            swap_out.at[h],
            swap_in.at[h],
            swap_send.at[h],
            swap_recv.at[h],
            device_id={"sp": mate},
            device_id_type=MESH,
        )

    def chain(h, c):
        rows = pl.ds(c * (dim // PIECES), dim // PIECES)
        return pltpu.make_async_remote_copy(
            chain_out.at[h, rows],
            chain_in.at[h, rows],
            chain_send.at[h, c],
            chain_recv.at[h, c],
            device_id={"sp": jnp.minimum(sp + 2, n_sp - 2 + odd)},
            device_id_type=MESH,
        )

    def summarise(h):
        hs = slice(h * dim, (h + 1) * dim)
        slack = slack_ref[:, hs]
        state, offset = None, None
        for b in range(blocks):
            ts = slice(b * SPAN, (b + 1) * SPAN)
            keyed = slack * (0.5 - 0.5 * jnp.tanh(0.5 * r_ref[ts, hs].astype(F32)))
            log_decay = jnp.log(1.0 - keyed) + extra[ts, h : h + 1]
            high = log_decay.astype(BF16)
            low = (log_decay - high.astype(F32)).astype(BF16)
            running = dot(tri2, jnp.concatenate([high, low], axis=0), ((1,), (0,)))
            end = running[SPAN - 1 :, :]
            probe = p_ref[ts, hs].astype(F32)
            query = probe * (0.5 + 0.5 * jnp.tanh(0.5 * probe))
            raised = query * jnp.exp(running)
            lifted[ts, hs] = raised.astype(BF16)
            lowered[ts, hs] = (keyed * jnp.exp(-running)).astype(BF16)
            sent = (keyed * jnp.exp(end - running)).astype(BF16)
            fresh = dot(v_ref[ts, hs], sent, ((0,), (0,)))
            if b == 0:
                lfull[ts, hs] = raised.astype(BF16)
                state, offset = fresh, end
            else:
                lfull[ts, hs] = (raised * jnp.exp(offset)).astype(BF16)
                inner[h, b - 1] = state.astype(BF16)
                state, offset = jnp.exp(end) * state + fresh, offset + end
        local[h] = state
        total = jnp.exp(offset)
        decay[h] = jnp.broadcast_to(total, (8, dim))
        high = total.astype(BF16)
        low = (total - high.astype(F32)).astype(BF16)
        swap_out[h, :dim, :] = state.astype(BF16)
        swap_out[h, dim:, :] = jnp.where(tag, high.astype(F32), low.astype(F32)).astype(BF16)

    def pass_on(h, arrival):
        swap(h).wait_recv()
        tail = swap_in[h, dim:, :].astype(F32)
        d_other, d_own = tail[0:1] + tail[1:2], decay[h, 0:1, :]
        is_odd = odd == 1
        d0 = jnp.where(is_odd, d_other, d_own)
        d1 = jnp.where(is_odd, d_own, d_other)
        for c in range(PIECES):
            rows = pl.ds(c * (dim // PIECES), dim // PIECES)
            other, own = swap_in[h, rows, :].astype(F32), local[h, rows, :]
            s0 = jnp.where(is_odd, other, own)
            s1 = jnp.where(is_odd, own, other)
            if arrival:
                chain(h, c).wait_recv()
            before = chain_in[h, rows, :].astype(F32)
            middle = d0 * before + s0
            chain_out[h, rows, :] = (d1 * middle + s1).astype(BF16)

            @pl.when(jnp.logical_not(last))
            def _():
                chain(h, c).start()

            enter[h, rows, :] = jnp.where(is_odd, middle, before).astype(BF16)

    def within(h):
        hs = slice(h * dim, (h + 1) * dim)
        for b in range(blocks):
            ts = slice(b * SPAN, (b + 1) * SPAN)
            up = lifted[ts, hs]
            scores = dot(up, lowered[ts, hs], ((1,), (1,)))
            scores = jnp.where(causal, scores, 0.0).astype(BF16)
            o = dot(scores, v_ref[ts, hs], ((1,), (0,)))
            if b > 0:
                o = o + dot(up, inner[h, b - 1], ((1,), (1,)))
            intra[ts, hs] = o

    gain = gain_ref[...]

    def close(h):
        hs = slice(h * dim, (h + 1) * dim)
        o = intra[:, hs] + dot(lfull[:, hs], enter[h], ((1,), (1,)))
        scale = lax.rsqrt(jnp.mean(o * o, axis=-1, keepdims=True) + 1e-6)
        normed[:, hs] = (o * scale * gain).astype(BF16)

    for g in range(groups):
        for c in loads[g]:
            c.wait()
        for h in range(g * GROUP, (g + 1) * GROUP):
            summarise(h)
        if g == 0:
            pl.semaphore_wait(barrier, 4 - first.astype(jnp.int32) - last.astype(jnp.int32))

        for h in range(g * GROUP, (g + 1) * GROUP):
            swap(h).start()

    for h in range(heads):
        within(h)

        @pl.when(first)
        def _():
            pass_on(h, False)

    theirs = pl.ds(pl.multiple_of((1 - tp) * half, half), half)
    mine = pl.ds(pl.multiple_of(tp * half, half), half)

    def exchange(t):
        ns = pl.ds(t * tile, tile)
        return pltpu.make_async_remote_copy(
            half_out.at[:, ns],
            half_in.at[:, ns],
            half_send.at[t],
            half_recv.at[t],
            device_id={"tp": 1 - tp},
            device_id_type=MESH,
        )

    for g in range(groups):
        hs = range(g * GROUP, (g + 1) * GROUP)

        ahead = range(heads if g == 0 else 0)

        @pl.when(jnp.logical_and(jnp.logical_not(first), jnp.logical_not(last)))
        def _():
            for h in ahead:
                pass_on(h, True)

        @pl.when(jnp.logical_and(jnp.logical_not(first), last))
        def _():
            for h in hs:
                pass_on(h, True)

        for h in hs:
            close(h)
        w_loads[g].wait()
        ks = slice(g * GROUP * dim, (g + 1) * GROUP * dim)
        if g < groups - 1:
            for t in range(TILES):
                ns = slice(t * tile, (t + 1) * tile)
                part = dot(normed[:, ks], w_ref[ks, ns], ((1,), (0,)))
                acc[:, ns] = part if g == 0 else acc[:, ns] + part
        else:
            for t in range(TILES):
                ns = slice(t * tile, (t + 1) * tile)
                part = dot(normed[theirs, ks], w_ref[ks, ns], ((1,), (0,)))
                if groups > 1:
                    part = part + acc[theirs, ns]
                half_out[:, ns] = part.astype(BF16)
                exchange(t).start()
            for t in range(TILES):
                ns = slice(t * tile, (t + 1) * tile)
                part = dot(normed[mine, ks], w_ref[ks, ns], ((1,), (0,)))
                if groups > 1:
                    part = part + acc[mine, ns]
                exchange(t).wait_recv()
                out_ref[:, ns] = (part + half_in[:, ns].astype(F32)).astype(BF16)

    for h in range(heads):
        swap(h).wait_send()

    @pl.when(jnp.logical_not(last))
    def _():
        for h in range(heads):
            for c in range(PIECES):
                chain(h, c).wait_send()

    for t in range(TILES):
        exchange(t).wait_send()


def body(n_sp, n_tp, p, r, v, x, slack, gain, w):
    tokens, channels = p.shape
    heads = x.shape[1]
    dim = channels // heads
    blocks = tokens // SPAN
    groups = heads // GROUP
    wide = w.shape[1]
    half = tokens // n_tp
    x, slack, gain = x.T, slack.reshape(1, channels), gain.reshape(1, dim)
    p, r, v, x, slack, gain, w = (
        pltpu.with_memory_space_constraint(a, pltpu.HBM) for a in (p, r, v, x, slack, gain, w)
    )
    vmem = pl.BlockSpec(memory_space=pltpu.VMEM)
    hbm = pl.BlockSpec(memory_space=pltpu.HBM)
    dma = pltpu.SemaphoreType.DMA
    return pl.pallas_call(
        functools.partial(kernel, n_sp),
        out_shape=jax.ShapeDtypeStruct((half, wide), BF16),
        in_specs=[hbm, hbm, hbm, vmem, vmem, vmem, hbm],
        out_specs=vmem,
        scratch_shapes=[
            pltpu.VMEM((tokens, channels), BF16),
            pltpu.VMEM((tokens, channels), BF16),
            pltpu.VMEM((tokens, channels), BF16),
            pltpu.VMEM(w.shape, BF16),
            pltpu.VMEM((tokens, channels), BF16),
            pltpu.VMEM((tokens, channels), BF16),
            pltpu.VMEM((tokens, channels), BF16),
            pltpu.VMEM((heads, max(blocks - 1, 1), dim, dim), BF16),
            pltpu.VMEM((heads, dim, dim), F32),
            pltpu.VMEM((heads, 8, dim), F32),
            pltpu.VMEM((tokens, channels), F32),
            pltpu.VMEM((heads, dim + 16, dim), BF16),
            pltpu.VMEM((heads, dim + 16, dim), BF16),
            pltpu.VMEM((heads, dim, dim), BF16),
            pltpu.VMEM((heads, dim, dim), BF16),
            pltpu.VMEM((heads, dim, dim), BF16),
            pltpu.VMEM((tokens, channels), BF16),
            pltpu.VMEM((tokens, wide), F32),
            pltpu.VMEM((half, wide), BF16),
            pltpu.VMEM((half, wide), BF16),
            dma((groups, 3)),
            dma((groups,)),
            dma((heads,)),
            dma((heads,)),
            dma((heads, PIECES)),
            dma((heads, PIECES)),
            dma((TILES,)),
            dma((TILES,)),
        ],
        compiler_params=pltpu.CompilerParams(
            collective_id=0, has_side_effects=True, vmem_limit_bytes=24 * 2**20
        ),
    )(p, r, v, x, slack, gain, w)


def solution(mesh):
    return jax.shard_map(
        functools.partial(body, mesh.shape["sp"], mesh.shape["tp"]),
        mesh=mesh,
        in_specs=(
            P(("grp", "sp"), "tp"),
            P(("grp", "sp"), "tp"),
            P(("grp", "sp"), "tp"),
            P(("grp", "sp"), "tp"),
            P("tp"),
            P(),
            P("tp", None),
        ),
        out_specs=P(("grp", "sp", "tp"), None),
        check_vma=False,
    )
```
